32 devices in a mesh: dp: 4 (over y, x), kv: 4 (over z), tp: 2 (over core).
Axes of the slice: x: 2, y: 2, z: 4, core: 2. Of those that a mesh axis runs over, the one named last changes fastest.
Arguments:
- tokens: bfloat16 [24, 4096], P('dp', 'kv'), may hold values from -64 to 64
- lengths: int32 [24], P('dp'), may hold values from 128 to 1024, as said below
- attn_gain: float32 [4096], P('kv'), may hold values from 0.1 to 1.9
- query_weight: bfloat16 [4096, 4096], P('kv', 'tp'), may hold values from -0.09375 to 0.09375
- key_weight: bfloat16 [4096, 256], P('kv', 'tp'), may hold values from -0.1875 to 0.1875
- value_weight: bfloat16 [4096, 256], P('kv', 'tp'), may hold values from -0.09375 to 0.09375
- forget_weight: bfloat16 [4096, 4], replicated, may hold values from -0.25 to 0.25
- forget_offset: float32 [4], P('tp'), may hold values from -6 to 0
- cache_keys: bfloat16 [24, 1024, 256], P('dp', 'kv', 'tp'), may hold values from -1600 to 1600
- cache_values: bfloat16 [24, 1024, 256], P('dp', 'kv', 'tp'), may hold values from -6 to 6
- gate_sum: float32 [24, 4, 1024], P('dp', 'tp', 'kv'), may hold values from -82 to 0
- out_weight: bfloat16 [4096, 4096], P('tp', 'kv'), may hold values from -0.1875 to 0.1875
- mlp_gain: float32 [4096], replicated, may hold values from 0.1 to 1.9
- up_weight: bfloat16 [4096, 16384], P(None, ('kv', 'tp')), may hold values from -0.09375 to 0.09375
- down_weight: bfloat16 [16384, 4096], P(('kv', 'tp')), may hold values from -0.0625 to 0.0625
Outputs:
- mixed: bfloat16 [24, 4096], P('dp', ('kv', 'tp'))
The draws below stay inside these ranges and needn't reach their ends.
Inputs may be any that keep to these rules, and one draw needn't show every extreme that they name: `lengths`: in every draw some sequence has all 1024 positions cached.
All inputs are finite; a program needn't handle non-finite values.
Results may differ from the reference program's by a relative error of at most 0.023.
Values may be sent and summed in bfloat16 or wider, within the bound.
No kernel may reach another device: no remote copies, remote signals or barrier semaphores. Data moves between devices by JAX's collectives and lax.ppermute only.
A program may use at most 128 MiB of HBM per device.

```python
import math
import jax
import jax.numpy as jnp
from jax import lax

D = 4096
HEADS = 64
HD = 64
KEY_VALUE_HEADS = 4
FF = 16384
CTX_DEV = 256
SEQUENCE_COUNT = 24
CTX = 1024
HEAD_GROUPS = 2


def seq_lengths(key):
    shorter = jax.random.randint(jax.random.fold_in(key, 11), (SEQUENCE_COUNT,), CTX // 8, CTX // 2 + 1)
    longer = jax.random.randint(jax.random.fold_in(key, 12), (SEQUENCE_COUNT,), CTX // 2, CTX + 1)
    shuffled = jax.random.permutation(jax.random.fold_in(key, 13), SEQUENCE_COUNT)
    ranking = jnp.argsort(shuffled)
    chosen = jnp.where(ranking < max(SEQUENCE_COUNT // 4, 1), longer, shorter)
    return jnp.where(ranking == 0, CTX, chosen).astype(jnp.int32)


def draw_lengths(key, part):
    return seq_lengths(key)


def draw_tokens(key, part):
    columns = jnp.arange(D, dtype=jnp.float32) / D - 0.5
    normal_draw = jnp.clip(jax.random.normal(jax.random.fold_in(key, 41), (SEQUENCE_COUNT, D), jnp.float32), -6.0, 6.0)
    column_scale = jnp.exp(math.log(10.0) * columns)
    row_factor = jnp.exp(jax.random.uniform(jax.random.fold_in(key, 42), (SEQUENCE_COUNT, 1), jnp.float32, -0.5 * math.log(10.0), 0.5 * math.log(10.0)))
    return (normal_draw * column_scale[None, :] * row_factor).astype(jnp.bfloat16)


def draw_gate_sum(key, part):
    lengths = seq_lengths(key)
    live_span = lengths.astype(jnp.float32)[:, None, None]
    token_offsets = jnp.arange(CTX)
    shuffled = jax.random.permutation(jax.random.fold_in(key, 21), KEY_VALUE_HEADS)
    slow_heads = (shuffled < KEY_VALUE_HEADS // 2)[None, :, None]
    blocks = CTX // CTX_DEV
    block_factor = jnp.exp(jax.random.uniform(jax.random.fold_in(key, 22), (SEQUENCE_COUNT, KEY_VALUE_HEADS, blocks), jnp.float32, -math.log(2.0), math.log(2.0)))
    block_factor = jnp.repeat(block_factor, CTX_DEV, axis=2)
    data_factor = jax.random.uniform(jax.random.fold_in(key, 23), (SEQUENCE_COUNT, KEY_VALUE_HEADS, CTX), jnp.float32, 0.5, 1.5)
    falloff_speeds = jnp.where(slow_heads, 0.5 / live_span, 1.0 / 40.0) * block_factor * data_factor
    spike_locations = jax.random.randint(jax.random.fold_in(key, 24), (SEQUENCE_COUNT, KEY_VALUE_HEADS, 3), 0, lengths[:, None, None])
    spike_penalty = jnp.log(1.0 - jax.random.uniform(jax.random.fold_in(key, 25), (SEQUENCE_COUNT, KEY_VALUE_HEADS, 3), jnp.float32, 0.2, 0.45))
    spike_events = jnp.sum(jnp.where(token_offsets[None, None, None, :] == spike_locations[..., None], spike_penalty[..., None], 0.0), axis=2)
    active_mask = token_offsets[None, None, :] < lengths[:, None, None]
    gate_logarithms = jnp.where(active_mask, spike_events - falloff_speeds, 0.0)
    return (jnp.sum(gate_logarithms, axis=2, keepdims=True) - jnp.cumsum(gate_logarithms, axis=2)).astype(jnp.float32)


def draw_cache_keys(key, part):
    drawn = 2.0 * jnp.clip(jax.random.normal(jax.random.fold_in(key, 31), (SEQUENCE_COUNT, CTX, KEY_VALUE_HEADS, HD), jnp.float32), -6.0, 6.0)
    return drawn.reshape(SEQUENCE_COUNT, CTX, KEY_VALUE_HEADS * HD).astype(jnp.bfloat16)


def spiked(result, rng, source, target, parts, factor):
    def block_of(dim):
        return (jnp.arange(result.shape[dim]) // (result.shape[dim] // parts)).reshape((-1,) + (1,) * (result.ndim - 1 - dim))

    one_side = jax.random.permutation(rng, parts)[block_of(target)]
    other_side = (block_of(target) + parts // 2) % parts
    return jnp.where((block_of(source) == one_side) | (block_of(source) == other_side), factor * result, result)


def steps_of(key, extent, cuts, low, high):
    def one(position, blocks):
        steps = jax.random.uniform(jax.random.fold_in(jax.random.fold_in(key, 6), position), (blocks,), jnp.float32, low / len(cuts), high / len(cuts))
        return jnp.repeat(jnp.exp(steps), extent[position] // blocks).reshape((-1,) + (1,) * (len(extent) - position - 1))

    level = one(*cuts[0])
    for cut in cuts[1:]:
        level = level * one(*cut)
    return level


def normal_values(key, shape, width, bound, cuts=(), held_as=jnp.bfloat16):
    values = width * jax.random.normal(key, shape, jnp.float32)
    if cuts:
        values = values * steps_of(key, shape, cuts, -0.22, 0.18)
    return jnp.clip(values, -bound, bound).astype(held_as)


def heavy_noise(rng, dims, deviation, reach, shards, heavy, kind=jnp.bfloat16):
    values = deviation * jax.random.normal(rng, dims, jnp.float32)
    if shards:
        values = values * steps_of(rng, dims, shards, -0.22, 0.18)
    return jnp.clip(spiked(values, jax.random.fold_in(rng, 3), *heavy), -reach, reach).astype(kind)


def setup_inputs(seed: int = 0) -> dict:
    arg_keys = jax.random.split(jax.random.key(seed), 16)
    return {
        "tokens": draw_tokens(jax.random.fold_in(arg_keys[15], 71), 0),
        "lengths": draw_lengths(jax.random.fold_in(arg_keys[15], 71), 0),
        "attn_gain": jnp.clip(1.0 + 0.18 * jax.random.normal(arg_keys[2], (D,), jnp.float32), 0.1, 1.9),
        "query_weight": normal_values(arg_keys[3], (D, HEADS * HD), D ** -0.5, 0.09375, ((0, 4), (1, 2))),
        "key_weight": normal_values(arg_keys[4], (D, KEY_VALUE_HEADS * HD), (D // 4) ** -0.5, 0.1875, ((0, 4), (1, 2))),
        "value_weight": normal_values(arg_keys[5], (D, KEY_VALUE_HEADS * HD), D ** -0.5, 0.09375, ((0, 4), (1, 2))),
        "forget_weight": normal_values(arg_keys[6], (D, KEY_VALUE_HEADS), (D // 8) ** -0.5, 0.25),
        "forget_offset": jnp.clip(-6.0 + 6.0 * jax.random.uniform(arg_keys[7], (KEY_VALUE_HEADS,), jnp.float32) ** steps_of(arg_keys[7], (KEY_VALUE_HEADS,), ((0, 2),), -0.2, 0.2), -6.0, 0.0),
        "cache_keys": draw_cache_keys(jax.random.fold_in(arg_keys[15], 71), 0),
        "cache_values": normal_values(arg_keys[9], (SEQUENCE_COUNT, CTX, KEY_VALUE_HEADS * HD), 1.0, 6.0, ((0, 4), (1, 4), (2, 2))),
        "gate_sum": draw_gate_sum(jax.random.fold_in(arg_keys[15], 71), 0),
        "out_weight": normal_values(arg_keys[11], (HEADS * HD, D), (D // 4) ** -0.5, 0.1875, ((0, 2), (1, 4))),
        "mlp_gain": jnp.clip(1.0 + 0.18 * jax.random.normal(arg_keys[12], (D,), jnp.float32), 0.1, 1.9),
        "up_weight": normal_values(arg_keys[13], (D, FF), D ** -0.5, 0.09375, ((1, 8),)),
        "down_weight": heavy_noise(arg_keys[14], (FF, D), FF ** -0.5, 0.0625, ((0, 8),), (0, 1, 8, 2.0)),
    }


epsilon = 1e-06

def reference(tokens, lengths, attn_gain, query_weight, key_weight, value_weight, forget_weight, forget_offset, cache_keys, cache_values, gate_sum, out_weight, mlp_gain, up_weight, down_weight):
    token_rows = tokens.astype(jnp.float32)
    row_scale = lax.rsqrt(lax.optimization_barrier(jnp.mean(token_rows * token_rows, axis=1, keepdims=True)) + epsilon)
    scaled_rows = (token_rows * attn_gain[None, :]).astype(jnp.bfloat16)
    queries = (jnp.dot(scaled_rows, query_weight, preferred_element_type=jnp.float32) * row_scale).astype(jnp.bfloat16)
    new_key = (jnp.dot(scaled_rows, key_weight, preferred_element_type=jnp.float32) * row_scale).astype(jnp.bfloat16)
    new_value = (jnp.dot(scaled_rows, value_weight, preferred_element_type=jnp.float32) * row_scale).astype(jnp.bfloat16)
    log_forget = jax.nn.log_sigmoid(jnp.dot(scaled_rows, forget_weight, preferred_element_type=jnp.float32) * row_scale + forget_offset[None, :])
    group_size = HEADS // KEY_VALUE_HEADS
    score_scale = HD ** (-0.5)
    token_offsets = jnp.arange(CTX)

    def one_sequence(inputs_one):
        query_row, key_rows, value_rows, gates, length, forget_row, own_key, own_value = inputs_one
        query_heads = query_row.astype(jnp.float32).reshape(KEY_VALUE_HEADS, group_size, HD)
        key_heads = key_rows.astype(jnp.float32).reshape(CTX, KEY_VALUE_HEADS, HD)
        value_heads = value_rows.astype(jnp.float32).reshape(CTX, KEY_VALUE_HEADS, HD)
        scores = jnp.einsum('kgd,pkd->kgp', query_heads, key_heads) * score_scale
        scores = scores + gates[:, None, :] + forget_row[:, None, None]
        active_mask = token_offsets < length
        scores = jnp.where(active_mask[None, None, :], scores, -jnp.inf)
        own_score = jnp.einsum('kgd,kd->kg', query_heads, own_key.astype(jnp.float32).reshape(KEY_VALUE_HEADS, HD)) * score_scale
        row_top = jnp.maximum(lax.optimization_barrier(jnp.max(scores, axis=2)), own_score)
        weight = jnp.exp(scores - row_top[..., None])
        own_weight = jnp.exp(own_score - row_top)
        totals = lax.optimization_barrier(jnp.sum(weight, axis=2)) + own_weight
        rounded = lax.optimization_barrier(weight.astype(jnp.bfloat16)).astype(jnp.float32)
        own_rounded = lax.optimization_barrier(own_weight.astype(jnp.bfloat16)).astype(jnp.float32)
        summed = jnp.einsum('kgp,pkd->kgd', rounded, value_heads)
        summed = summed + own_rounded[..., None] * own_value.astype(jnp.float32).reshape(KEY_VALUE_HEADS, 1, HD)
        return (summed / totals[..., None]).reshape(HEADS * HD).astype(jnp.bfloat16)
    attended = lax.map(one_sequence, (queries, cache_keys, cache_values, gate_sum, lengths, log_forget, new_key, new_value))
    group_width = HEADS * HD // HEAD_GROUPS
    summed_mid = token_rows
    for group_index in range(HEAD_GROUPS):
        partial_value = jnp.dot(attended[:, group_index * group_width:(group_index + 1) * group_width], out_weight[group_index * group_width:(group_index + 1) * group_width], preferred_element_type=jnp.float32)
        partial_value = lax.optimization_barrier(partial_value.astype(jnp.bfloat16)).astype(jnp.float32)
        summed_mid = summed_mid + partial_value
    mid_rows = summed_mid.astype(jnp.bfloat16)
    mid_wide = mid_rows.astype(jnp.float32)
    normed_mid = (mid_wide * mlp_gain[None, :] * lax.rsqrt(lax.optimization_barrier(jnp.mean(mid_wide * mid_wide, axis=1, keepdims=True)) + epsilon)).astype(jnp.bfloat16)
    hidden = jnp.square(jax.nn.relu(jnp.dot(normed_mid, up_weight, preferred_element_type=jnp.float32))).astype(jnp.bfloat16)
    return (mid_wide + jnp.dot(hidden, down_weight, preferred_element_type=jnp.float32)).astype(jnp.bfloat16)
```

```python
import functools
import jax
import jax.numpy as jnp
from jax import lax
from jax.experimental import pallas as pl
from jax.experimental.pallas import tpu as pltpu
from jax.sharding import PartitionSpec as P

D = 4096
HEADS = 64
HD = 64
KEY_VALUE_HEADS = 4


epsilon = 1e-06
floor_score = -1e30


def combined_all(x, axis, combine):
    everything = jax.tree.map(
        lambda part, kind: lax.all_gather(part.astype(kind), axis),
        x,
        (jnp.bfloat16, jnp.bfloat16, jnp.bfloat16),
    )

    def take(k):
        return jax.tree.map(lambda part, own: part[k].astype(own.dtype), everything, x)

    return lax.fori_loop(
        1, lax.axis_size(axis), lambda k, so_far: combine(so_far, take(k)), take(0)
    )


def combine_parts(earlier, later):
    first_top, first_total, first_values = earlier
    second_top, second_total, second_values = later
    merged_top = jnp.maximum(first_top, second_top)
    first_scale = jnp.exp(first_top - merged_top)
    second_scale = jnp.exp(second_top - merged_top)
    first_wide = jnp.repeat(first_scale, HD, axis=1)
    second_wide = jnp.repeat(second_scale, HD, axis=1)
    return (
        merged_top,
        first_total * first_scale + second_total * second_scale,
        first_values * first_wide + second_values * second_wide,
    )


def shards(
    tokens,
    lengths,
    attn_gain,
    query_weight,
    key_weight,
    value_weight,
    forget_weight,
    forget_offset,
    cache_keys,
    cache_values,
    gate_sum,
    out_weight,
    mlp_gain,
    up_weight,
    down_weight,
):
    row_count = tokens.shape[0]
    feature_cols = tokens.shape[1]
    kv_place = lax.axis_index("kv")
    tp_place = lax.axis_index("tp")
    local_heads = key_weight.shape[1] // HD
    group_size = HEADS // KEY_VALUE_HEADS
    token_rows = tokens.astype(jnp.float32)
    scaled_rows = (token_rows * attn_gain[None, :]).astype(jnp.bfloat16)
    square_part = jnp.sum(token_rows * token_rows, axis=1)
    query_part = jnp.dot(scaled_rows, query_weight, preferred_element_type=jnp.float32)
    key_part = jnp.dot(scaled_rows, key_weight, preferred_element_type=jnp.float32)
    value_part = jnp.dot(scaled_rows, value_weight, preferred_element_type=jnp.float32)
    gate_rows = lax.dynamic_slice(
        forget_weight,
        (kv_place * feature_cols, tp_place * local_heads),
        (feature_cols, local_heads),
    )
    forget_part = jnp.dot(scaled_rows, gate_rows, preferred_element_type=jnp.float32)
    query_sum, key_sum, value_sum, forget_sum, square_sum = lax.psum(
        (query_part, key_part, value_part, forget_part, square_part), "kv"
    )
    row_scale = lax.rsqrt(square_sum / D + epsilon)[:, None]
    queries = (query_sum * row_scale).astype(jnp.bfloat16)
    new_key = (key_sum * row_scale).astype(jnp.bfloat16)
    new_value = (value_sum * row_scale).astype(jnp.bfloat16)
    log_forget = jax.nn.log_sigmoid(forget_sum * row_scale + forget_offset[None, :])
    positions_here = cache_keys.shape[1]
    key_heads = cache_keys.reshape(row_count, positions_here, local_heads, HD)
    value_heads = cache_values.reshape(row_count, positions_here, local_heads, HD)
    query_heads = queries.reshape(row_count, local_heads, group_size, HD)
    scores = jnp.einsum(
        "skgd,spkd->skgp", query_heads, key_heads, preferred_element_type=jnp.float32
    ) * HD ** (-0.5)
    scores = scores + gate_sum[:, :, None, :] + log_forget[:, :, None, None]
    cache_pos = kv_place * positions_here + jnp.arange(positions_here)
    active_mask = (cache_pos[None, :] < lengths[:, None])[:, None, None, :]
    local_top = jnp.max(jnp.where(active_mask, scores, floor_score), axis=3)
    weights = jnp.where(active_mask, jnp.exp(scores - local_top[..., None]), 0.0)
    local_total = jnp.sum(weights, axis=3)
    local_values = jnp.einsum(
        "skgp,spkd->skgd",
        weights.astype(jnp.bfloat16),
        value_heads,
        preferred_element_type=jnp.float32,
    )
    head_cols = local_heads * group_size
    merged_top, merged_total, merged_values = combined_all(
        (
            local_top.reshape(row_count, head_cols),
            local_total.reshape(row_count, head_cols),
            local_values.reshape(row_count, head_cols * HD),
        ),
        "kv",
        combine_parts,
    )
    own_score = jnp.einsum(
        "skgd,skd->skg",
        query_heads,
        new_key.reshape(row_count, local_heads, HD),
        preferred_element_type=jnp.float32,
    ).reshape(row_count, head_cols) * HD ** (-0.5)
    final_top = jnp.maximum(merged_top, own_score)
    past_scale = jnp.exp(merged_top - final_top)
    own_weight = jnp.exp(own_score - final_top)
    totals = merged_total * past_scale + own_weight
    own_rounded = lax.optimization_barrier(own_weight.astype(jnp.bfloat16)).astype(jnp.float32)
    own_values = jnp.broadcast_to(
        new_value.astype(jnp.float32).reshape(row_count, local_heads, 1, HD),
        (row_count, local_heads, group_size, HD),
    ).reshape(row_count, head_cols * HD)
    weighted = (
        merged_values * jnp.repeat(past_scale, HD, axis=1)
        + jnp.repeat(own_rounded, HD, axis=1) * own_values
    )
    attended = (weighted / jnp.repeat(totals, HD, axis=1)).astype(jnp.bfloat16)
    partial_out = jnp.dot(attended, out_weight, preferred_element_type=jnp.float32)
    head_sum = lax.psum(partial_out.astype(jnp.bfloat16), "tp").astype(jnp.float32)
    mid_cols = (token_rows + head_sum).astype(jnp.bfloat16)
    mid_rows = lax.all_gather(mid_cols, "kv", axis=1, tiled=True)
    mid_wide = mid_rows.astype(jnp.float32)
    normed_mid = (
        mid_wide
        * mlp_gain[None, :]
        * lax.rsqrt(jnp.mean(mid_wide * mid_wide, axis=1, keepdims=True) + epsilon)
    ).astype(jnp.bfloat16)
    hidden = jnp.square(
        jax.nn.relu(jnp.dot(normed_mid, up_weight, preferred_element_type=jnp.float32))
    ).astype(jnp.bfloat16)
    mixer_term = jnp.dot(hidden, down_weight, preferred_element_type=jnp.float32)
    kv_count = lax.axis_size("kv")
    tp_count = lax.axis_size("tp")
    block_cols = mixer_term.shape[1] // (kv_count * tp_count)
    reordered = (
        mixer_term.reshape(row_count, kv_count, tp_count, block_cols)
        .transpose(0, 2, 1, 3)
        .reshape(row_count, kv_count * tp_count * block_cols)
    )
    pair_share = lax.psum_scatter(
        reordered.astype(jnp.bfloat16), "tp", scatter_dimension=1, tiled=True
    ).astype(jnp.float32)
    mixer_share = lax.psum_scatter(pair_share, "kv", scatter_dimension=1, tiled=True)
    out_cols = mixer_share.shape[1]
    start_col = (kv_place * tp_count + tp_place) * out_cols
    mid_share = lax.dynamic_slice_in_dim(mid_wide, start_col, out_cols, 1)
    return (mid_share + mixer_share).astype(jnp.bfloat16)


LANES = 128
SUBLANES = 8
VMEM = pltpu.VMEM
HBM = pltpu.HBM
f32 = jnp.float32
bf16 = jnp.bfloat16
in_vmem = pl.BlockSpec(memory_space=pltpu.VMEM)
in_smem = pl.BlockSpec(memory_space=pltpu.SMEM)
in_hbm = pl.BlockSpec(memory_space=pltpu.HBM)
anywhere = pl.BlockSpec(memory_space=pl.ANY)


def call(kernel, outs, in_specs, args, scratch=(), megabytes=8, weight_bytes=0, name=None):
    many = isinstance(outs, (list, tuple))
    return pl.pallas_call(
        kernel,
        out_shape=outs,
        in_specs=in_specs,
        out_specs=[in_vmem] * len(outs) if many else in_vmem,
        scratch_shapes=list(scratch),
        compiler_params=pltpu.CompilerParams(vmem_limit_bytes=megabytes * 1024 * 1024),
        cost_estimate=pl.CostEstimate(
            flops=12 * max(weight_bytes, 1 << 16),
            bytes_accessed=max(weight_bytes, 1 << 16),
            transcendentals=0,
        ),
        name=name,
    )(*args)


def pinned(x, space):
    return pltpu.with_memory_space_constraint(x, space)


def round_up(n, m):
    return -(-n // m) * m


def lane_index(rows):
    return lax.broadcasted_iota(jnp.int32, (rows, LANES), 1)


def project_kernel(
    tokens_hbm,
    gain_hbm,
    query_hbm,
    key_hbm,
    value_hbm,
    forget_hbm,
    part_ref,
    tokens,
    gain,
    query,
    key,
    value,
    forget,
    stage,
    sems,
):
    rows, feats = tokens.shape
    chunks = query.shape[0]
    depth = query.shape[1]
    kv_place = lax.axis_index("kv")
    start = pl.multiple_of(kv_place * feats, feats)
    copies = [
        pltpu.make_async_copy(tokens_hbm, tokens, sems.at[0]),
        pltpu.make_async_copy(gain_hbm, gain, sems.at[1]),
        pltpu.make_async_copy(forget_hbm.at[pl.ds(start, feats), :], forget, sems.at[2]),
        pltpu.make_async_copy(key_hbm, key, sems.at[3]),
        pltpu.make_async_copy(value_hbm, value, sems.at[4]),
    ]
    streams = [
        pltpu.make_async_copy(
            query_hbm.at[pl.ds(i * depth, depth), :], query.at[i], sems.at[5 + i]
        )
        for i in range(chunks)
    ]
    for copy in copies[:2]:
        copy.start()
    for copy in streams:
        copy.start()
    for copy in copies[2:]:
        copy.start()
    for copy in copies[:2]:
        copy.wait()
    token_rows = tokens[...].astype(f32)
    scaled = (token_rows * gain[...]).astype(bf16)
    squares = jnp.sum(token_rows * token_rows, axis=1, keepdims=True)
    total = None
    for i in range(chunks):
        streams[i].wait()
        term = jnp.dot(
            scaled[:, i * depth : (i + 1) * depth], query[i], preferred_element_type=f32
        )
        total = term if total is None else total + term
    for copy in copies[2:]:
        copy.wait()
    key_part = jnp.dot(scaled, key[...], preferred_element_type=f32)
    value_part = jnp.dot(scaled, value[...], preferred_element_type=f32)
    forget_part = jnp.dot(scaled, forget[...], preferred_element_type=f32)
    heads = forget_part.shape[1]
    lane = lane_index(rows)
    extra = jnp.where(lane == heads, squares, 0.0)
    for j in range(heads):
        extra = jnp.where(lane == j, forget_part[:, j : j + 1], extra)
    high = extra.astype(bf16).astype(f32)
    low = extra - high
    extra = high + pltpu.roll(low, LANES // 2, axis=1)
    stage[...] = jnp.zeros(stage.shape, f32)
    tiles = total.shape[1] // LANES
    for c in range(tiles):
        stage[c * rows : (c + 1) * rows, :] = total[:, c * LANES : (c + 1) * LANES]
    for j, block in enumerate((key_part, value_part, extra)):
        stage[(tiles + j) * rows : (tiles + j + 1) * rows, :] = block
    part_ref[...] = stage[...].astype(bf16)


def hold_kernel(count, *refs):
    sources = refs[1 : 1 + count]
    targets = refs[1 + count : 1 + 2 * count]
    sems = refs[1 + 2 * count]
    copies = [
        pltpu.make_async_copy(s, t, sems.at[i])
        for i, (s, t) in enumerate(zip(sources, targets))
    ]
    for copy in copies:
        copy.start()
    for copy in copies:
        copy.wait()


def hold(after, arrays, name):
    outs = [pltpu.VMEM(a.shape, a.dtype) for a in arrays]
    size = sum(a.size * a.dtype.itemsize for a in arrays)
    return call(
        functools.partial(hold_kernel, len(arrays)),
        outs,
        [anywhere] + [in_hbm] * len(arrays),
        [after] + [pinned(a, HBM) for a in arrays],
        scratch=[pltpu.SemaphoreType.DMA((len(arrays),))],
        megabytes=1,
        weight_bytes=size,
        name=name,
    )


def hold_rows_kernel(first, count, pieces, _, source, target, sems):
    depth = count // pieces
    copies = [
        pltpu.make_async_copy(
            source.at[pl.ds(first + i * depth, depth), :],
            target.at[pl.ds(i * depth, depth), :],
            sems.at[i],
        )
        for i in range(pieces)
    ]
    for copy in copies:
        copy.start()
    for copy in copies:
        copy.wait()


def hold_rows(after, array, first, count, name):
    pieces = 4
    return call(
        functools.partial(hold_rows_kernel, first, count, pieces),
        pltpu.VMEM((count, array.shape[1]), array.dtype),
        [anywhere, in_hbm],
        [after, pinned(array, HBM)],
        scratch=[pltpu.SemaphoreType.DMA((pieces,))],
        megabytes=1,
        weight_bytes=count * array.shape[1] * array.dtype.itemsize,
        name=name,
    )


def attend_kernel(
    peers, rows, lengths, offset, keys, values, gates, *refs
):
    parts = refs[:peers]
    sent_ref, stage = refs[peers:]
    positions = keys.shape[1]
    kv_place = lax.axis_index("kv")
    tp_place = lax.axis_index("tp")
    summed = parts[0][...].astype(f32)
    for part in parts[1:]:
        summed = summed + part[...].astype(f32)
    stage[...] = summed
    tiles = HEADS // lax.axis_size("tp") * HD // LANES
    half = tiles // 2
    extra = stage[(tiles + 2) * rows : (tiles + 3) * rows, :]
    extra = extra + pltpu.roll(extra, LANES // 2, axis=1)
    scale = lax.rsqrt(extra[:, KEY_VALUE_HEADS : KEY_VALUE_HEADS + 1] / D + epsilon)
    gate_in = extra * scale
    lane_row = lax.broadcasted_iota(jnp.int32, (tiles, LANES), 1)
    tile_row = lax.broadcasted_iota(jnp.int32, (tiles, LANES), 0)
    low_lane = lane_row < HD
    low_tile = tile_row < half
    mine = low_lane == low_tile
    wide_tile = lax.broadcasted_iota(jnp.int32, (tiles, positions), 0) < half
    place = kv_place * positions + lax.broadcasted_iota(jnp.int32, (2 * tiles, positions), 1)
    owner = kv_place == 0
    stats = jnp.zeros((tiles, LANES), f32)
    for b in range(rows):
        row_scale = scale[b : b + 1, :]
        tile = (stage[pl.ds(b, tiles, stride=rows), :] * row_scale).astype(bf16).astype(f32)
        turned = pltpu.roll(tile, HD, axis=1)
        even = jnp.where(low_tile, tile, turned)
        odd = jnp.where(low_tile, turned, tile)
        even = jnp.where(mine, even, 0.0)
        odd = jnp.where(mine, odd, 0.0)
        query = jnp.concatenate([even, odd], axis=0)
        new_key = (stage[tiles * rows + b : tiles * rows + b + 1, :] * row_scale).astype(bf16)
        new_value = (
            stage[(tiles + 1) * rows + b : (tiles + 1) * rows + b + 1, :] * row_scale
        ).astype(bf16)
        scores = lax.dot_general(
            query.astype(bf16),
            keys[b],
            (((1,), (1,)), ((), ())),
            preferred_element_type=f32,
        ) * HD ** (-0.5)
        both = []
        for g in range(2):
            column = tp_place * 2 + g
            picked = jnp.sum(
                jnp.where(
                    lax.broadcasted_iota(jnp.int32, (1, LANES), 1) == column,
                    gate_in[b : b + 1, :],
                    0.0,
                ),
                axis=1,
                keepdims=True,
            )
            raw = picked + offset[g]
            log_forget = jnp.minimum(raw, 0.0) - jnp.log1p(jnp.exp(-jnp.abs(raw)))
            both.append(gates[b, g : g + 1, :] + log_forget)
        bias = jnp.where(wide_tile, both[0], both[1])
        scores = scores + jnp.concatenate([bias, bias], axis=0)
        live = place < lengths[b]
        scores = jnp.where(live, scores, floor_score)
        own = jnp.sum(query * new_key.astype(f32), axis=1, keepdims=True) * HD ** (-0.5)
        own = jnp.where(owner, own, floor_score)
        top = jnp.maximum(jnp.max(scores, axis=1, keepdims=True), own)
        top_high = top.astype(bf16).astype(f32)
        top_low = (top - top_high).astype(bf16).astype(f32)
        top = top_high + top_low
        weights = jnp.where(live, jnp.exp(scores - top), 0.0)
        own_weight = jnp.where(owner, jnp.exp(own - top), 0.0)
        total = jnp.sum(weights, axis=1, keepdims=True) + own_weight
        total_high = total.astype(bf16).astype(f32)
        total_low = total - total_high
        summed_values = jnp.dot(weights.astype(bf16), values[b], preferred_element_type=f32)
        summed_values = summed_values + own_weight.astype(bf16).astype(f32) * new_value.astype(f32)
        even = summed_values[:tiles]
        odd = summed_values[tiles:]
        placed_even = jnp.where(low_tile, even, pltpu.roll(even, HD, axis=1))
        placed_odd = jnp.where(low_tile, pltpu.roll(odd, HD, axis=1), odd)
        sent_ref[b * tiles : (b + 1) * tiles, :] = jnp.where(
            low_lane, placed_even, placed_odd
        ).astype(bf16)
        for j, column in enumerate((top_high, top_low, total_high, total_low)):
            for parity in range(2):
                stats = jnp.where(
                    lane_row == j * (LANES // 4) + 2 * b + parity,
                    column[parity * tiles : (parity + 1) * tiles],
                    stats,
                )
    sent_ref[rows * tiles :, :] = stats.astype(bf16)


def output_kernel(peers, rows, weight, tokens, _, *refs):
    parts = refs[:peers]
    partial_ref, kept_ref, stage = refs[peers:]
    tiles = parts[0].shape[0] // (rows + 1)
    quarter = LANES // 4
    tops, totals = [], []
    for part in parts:
        stats = part[rows * tiles :, :].astype(f32)
        tops.append(stats + pltpu.roll(stats, LANES - quarter, axis=1))
        totals.append(
            pltpu.roll(stats, LANES - 2 * quarter, axis=1)
            + pltpu.roll(stats, LANES - 3 * quarter, axis=1)
        )
    top = functools.reduce(jnp.maximum, tops)
    scales = [jnp.exp(t - top) for t in tops]
    total = functools.reduce(jnp.add, [t * s for t, s in zip(totals, scales)])
    shares = [s / total for s in scales]
    low_lane = lane_index(tiles) < HD
    for b in range(rows):
        mixed = None
        for part, share in zip(parts, shares):
            factor = jnp.where(
                low_lane, share[:, 2 * b : 2 * b + 1], share[:, 2 * b + 1 : 2 * b + 2]
            )
            term = part[b * tiles : (b + 1) * tiles, :].astype(f32) * factor
            mixed = term if mixed is None else mixed + term
        stage[b * tiles : (b + 1) * tiles, :] = mixed
    attended = jnp.concatenate(
        [stage[pl.ds(c, rows, stride=tiles), :] for c in range(tiles)], axis=1
    ).astype(bf16)
    partial = jnp.dot(attended, weight[...], preferred_element_type=f32).astype(bf16)
    partial_ref[...] = partial
    kept_ref[...] = tokens[...].astype(f32) + partial.astype(f32)


def mixer_kernel(
    peers, gain, up_low, up_high, down_hbm, *refs
):
    mids = refs[:peers]
    kept_ref, sent_ref, down, normed, spread, sems = refs[peers:]
    rows, width = mids[0].shape
    chunks, depth = down.shape[:2]
    kv_place = lax.axis_index("kv")
    tp_place = lax.axis_index("tp")
    streams = [
        pltpu.make_async_copy(
            down_hbm.at[pl.ds(i * depth, depth), :], down.at[i], sems.at[i]
        )
        for i in range(chunks)
    ]
    for copy in streams:
        copy.start()
    wides = [m[...].astype(f32) for m in mids]
    squares = functools.reduce(
        jnp.add, [jnp.sum(w * w, axis=1, keepdims=True) for w in wides]
    )
    scale = lax.rsqrt(squares / D + epsilon)
    for k in range(peers):
        source = kv_place ^ k
        normed[source] = wides[k] * gain[source] * scale
    half = peers // 2
    hidden = None
    for j in range(peers):
        up = up_low if j < half else up_high
        first = (j % half) * width
        term = jnp.dot(
            normed[j].astype(bf16), up[first : first + width, :], preferred_element_type=f32
        )
        hidden = term if hidden is None else hidden + term
    hidden = jnp.square(jnp.maximum(hidden, 0.0)).astype(bf16)
    total = None
    for i in range(chunks):
        streams[i].wait()
        term = jnp.dot(
            hidden[:, i * depth : (i + 1) * depth], down[i], preferred_element_type=f32
        )
        total = term if total is None else total + term
    blocks = spread.shape[0]
    cols = spread.shape[2]
    for q in range(blocks):
        spread[q] = total[:, q * cols : (q + 1) * cols]
    for k in range(peers):
        target = 2 * (kv_place ^ k)
        kept_ref[k] = spread[target + tp_place]
        sent_ref[k] = spread[target + 1 - tp_place].astype(bf16)
    for half_place in range(2):

        @pl.when(tp_place == half_place)
        def _():
            kept_ref[0] += mids[0][:, half_place * cols : (half_place + 1) * cols].astype(f32)


def swap(x, axis, k):
    return lax.ppermute(x, axis, [(i, i ^ k) for i in range(lax.axis_size(axis))])


def shards_direct(
    tokens,
    lengths,
    attn_gain,
    query_weight,
    key_weight,
    value_weight,
    forget_weight,
    forget_offset,
    cache_keys,
    cache_values,
    gate_sum,
    out_weight,
    mlp_gain,
    up_weight,
    down_weight,
):
    rows, feats = tokens.shape
    peers = lax.axis_size("kv")
    others = range(1, peers)
    tiles = query_weight.shape[1] // LANES
    chunks = 4
    depth = feats // chunks
    part_rows = round_up((tiles + 3) * rows, SUBLANES)
    part = call(
        project_kernel,
        jax.ShapeDtypeStruct((part_rows, LANES), bf16),
        [in_hbm] * 6,
        [
            pinned(x, HBM)
            for x in (
                tokens,
                attn_gain.reshape(1, feats),
                query_weight,
                key_weight,
                value_weight,
                forget_weight,
            )
        ],
        scratch=[
            pltpu.VMEM((rows, feats), bf16),
            pltpu.VMEM((1, feats), f32),
            pltpu.VMEM((chunks, depth, query_weight.shape[1]), bf16),
            pltpu.VMEM(key_weight.shape, bf16),
            pltpu.VMEM(value_weight.shape, bf16),
            pltpu.VMEM((feats, forget_weight.shape[1]), bf16),
            pltpu.VMEM((part_rows, LANES), f32),
            pltpu.SemaphoreType.DMA((5 + chunks,)),
        ],
        megabytes=12,
        weight_bytes=query_weight.size * 2,
        name="project",
    )
    parts = [part] + [swap(part, "kv", k) for k in others]
    keys_held, values_held, gates_held, out_held, tokens_held = hold(
        part, [cache_keys, cache_values, gate_sum, out_weight, tokens], "hold_caches"
    )
    sent = call(
        functools.partial(attend_kernel, peers, rows),
        jax.ShapeDtypeStruct(((rows + 1) * tiles, LANES), bf16),
        [in_smem] * 2 + [in_vmem] * (3 + peers),
        [lengths, forget_offset]
        + [pinned(x, VMEM) for x in (keys_held, values_held, gates_held)]
        + parts,
        scratch=[pltpu.VMEM((part_rows, LANES), f32)],
        megabytes=6,
        name="attend",
    )
    sents = [sent] + [swap(sent, "kv", k) for k in others]
    total_rows = up_weight.shape[0]
    up_low = hold_rows(sent, up_weight, 0, total_rows // 2, "hold_low")
    partial, kept = call(
        functools.partial(output_kernel, peers, rows),
        [
            jax.ShapeDtypeStruct((rows, out_weight.shape[1]), bf16),
            jax.ShapeDtypeStruct((rows, out_weight.shape[1]), f32),
        ],
        [in_vmem] * 2 + [anywhere] + [in_vmem] * peers,
        [pinned(out_held, VMEM), pinned(tokens_held, VMEM), pinned(up_low, VMEM)] + sents,
        scratch=[pltpu.VMEM((rows * tiles, LANES), f32)],
        megabytes=6,
        name="output",
    )
    mid = (kept + swap(partial, "tp", 1).astype(f32)).astype(bf16)
    mids = [mid] + [swap(mid, "kv", k) for k in others]
    up_high = hold_rows(mid, up_weight, total_rows // 2, total_rows // 2, "hold_high")
    hidden_rows, model = down_weight.shape
    pieces = 8
    blocks = 2 * peers
    cols = model // blocks
    kept, crossing = call(
        functools.partial(mixer_kernel, peers),
        [
            jax.ShapeDtypeStruct((peers, rows, cols), f32),
            jax.ShapeDtypeStruct((peers, rows, cols), bf16),
        ],
        [in_vmem] * 3 + [in_hbm] + [in_vmem] * peers,
        [
            mlp_gain.reshape(peers, 1, model // peers),
            pinned(up_low, VMEM),
            pinned(up_high, VMEM),
            pinned(down_weight, HBM),
        ]
        + mids,
        scratch=[
            pltpu.VMEM((pieces, hidden_rows // pieces, model), bf16),
            pltpu.VMEM((peers, rows, model // peers), f32),
            pltpu.VMEM((blocks, rows, cols), f32),
            pltpu.SemaphoreType.DMA((pieces,)),
        ],
        megabytes=24,
        weight_bytes=down_weight.size * 2,
        name="mixer",
    )
    paired = kept + swap(crossing, "tp", 1).astype(f32)
    shares = [swap(paired[k].astype(bf16), "kv", k) for k in others]
    result = paired[0]
    for share in shares:
        result = result + share.astype(f32)
    return result.astype(bf16)


def direct_fits(mesh):
    peers = mesh.shape["kv"]
    return mesh.shape["tp"] == 2 and peers in (2, 4) and HD * 2 == LANES


def solution(mesh):
    placed = (
        P("dp", "kv"),
        P("dp"),
        P("kv"),
        P("kv", "tp"),
        P("kv", "tp"),
        P("kv", "tp"),
        P(),
        P("tp"),
        P("dp", "kv", "tp"),
        P("dp", "kv", "tp"),
        P("dp", "tp", "kv"),
        P("tp", "kv"),
        P(),
        P(None, ("kv", "tp")),
        P(("kv", "tp"), None),
    )
    return jax.shard_map(
        shards_direct if direct_fits(mesh) else shards, mesh=mesh, in_specs=placed, out_specs=P("dp", ("kv", "tp")), check_vma=False
    )
```

```python
import functools
import jax
import jax.numpy as jnp
from jax import lax
from jax.experimental import pallas as pl
from jax.experimental.pallas import tpu as pltpu
from jax.sharding import PartitionSpec as P

D = 4096
HEADS = 64
HD = 64
KEY_VALUE_HEADS = 4


epsilon = 1e-06
floor_score = -1e30


def combined_all(x, axis, combine):
    everything = jax.tree.map(
        lambda part, kind: lax.all_gather(part.astype(kind), axis),
        x,
        (jnp.bfloat16, jnp.bfloat16, jnp.bfloat16),
    )

    def take(k):
        return jax.tree.map(lambda part, own: part[k].astype(own.dtype), everything, x)

    return lax.fori_loop(
        1, lax.axis_size(axis), lambda k, so_far: combine(so_far, take(k)), take(0)
    )


def combine_parts(earlier, later):
    first_top, first_total, first_values = earlier
    second_top, second_total, second_values = later
    merged_top = jnp.maximum(first_top, second_top)
    first_scale = jnp.exp(first_top - merged_top)
    second_scale = jnp.exp(second_top - merged_top)
    first_wide = jnp.repeat(first_scale, HD, axis=1)
    second_wide = jnp.repeat(second_scale, HD, axis=1)
    return (
        merged_top,
        first_total * first_scale + second_total * second_scale,
        first_values * first_wide + second_values * second_wide,
    )


def shards(
    tokens,
    lengths,
    attn_gain,
    query_weight,
    key_weight,
    value_weight,
    forget_weight,
    forget_offset,
    cache_keys,
    cache_values,
    gate_sum,
    out_weight,
    mlp_gain,
    up_weight,
    down_weight,
):
    row_count = tokens.shape[0]
    feature_cols = tokens.shape[1]
    kv_place = lax.axis_index("kv")
    tp_place = lax.axis_index("tp")
    local_heads = key_weight.shape[1] // HD
    group_size = HEADS // KEY_VALUE_HEADS
    token_rows = tokens.astype(jnp.float32)
    scaled_rows = (token_rows * attn_gain[None, :]).astype(jnp.bfloat16)
    square_part = jnp.sum(token_rows * token_rows, axis=1)
    query_part = jnp.dot(scaled_rows, query_weight, preferred_element_type=jnp.float32)
    key_part = jnp.dot(scaled_rows, key_weight, preferred_element_type=jnp.float32)
    value_part = jnp.dot(scaled_rows, value_weight, preferred_element_type=jnp.float32)
    gate_rows = lax.dynamic_slice(
        forget_weight,
        (kv_place * feature_cols, tp_place * local_heads),
        (feature_cols, local_heads),
    )
    forget_part = jnp.dot(scaled_rows, gate_rows, preferred_element_type=jnp.float32)
    query_sum, key_sum, value_sum, forget_sum, square_sum = lax.psum(
        (query_part, key_part, value_part, forget_part, square_part), "kv"
    )
    row_scale = lax.rsqrt(square_sum / D + epsilon)[:, None]
    queries = (query_sum * row_scale).astype(jnp.bfloat16)
    new_key = (key_sum * row_scale).astype(jnp.bfloat16)
    new_value = (value_sum * row_scale).astype(jnp.bfloat16)
    log_forget = jax.nn.log_sigmoid(forget_sum * row_scale + forget_offset[None, :])
    positions_here = cache_keys.shape[1]
    key_heads = cache_keys.reshape(row_count, positions_here, local_heads, HD)
    value_heads = cache_values.reshape(row_count, positions_here, local_heads, HD)
    query_heads = queries.reshape(row_count, local_heads, group_size, HD)
    scores = jnp.einsum(
        "skgd,spkd->skgp", query_heads, key_heads, preferred_element_type=jnp.float32
    ) * HD ** (-0.5)
    scores = scores + gate_sum[:, :, None, :] + log_forget[:, :, None, None]
    cache_pos = kv_place * positions_here + jnp.arange(positions_here)
    active_mask = (cache_pos[None, :] < lengths[:, None])[:, None, None, :]
    local_top = jnp.max(jnp.where(active_mask, scores, floor_score), axis=3)
    weights = jnp.where(active_mask, jnp.exp(scores - local_top[..., None]), 0.0)
    local_total = jnp.sum(weights, axis=3)
    local_values = jnp.einsum(
        "skgp,spkd->skgd",
        weights.astype(jnp.bfloat16),
        value_heads,
        preferred_element_type=jnp.float32,
    )
    head_cols = local_heads * group_size
    merged_top, merged_total, merged_values = combined_all(
        (
            local_top.reshape(row_count, head_cols),
            local_total.reshape(row_count, head_cols),
            local_values.reshape(row_count, head_cols * HD),
        ),
        "kv",
        combine_parts,
    )
    own_score = jnp.einsum(
        "skgd,skd->skg",
        query_heads,
        new_key.reshape(row_count, local_heads, HD),
        preferred_element_type=jnp.float32,
    ).reshape(row_count, head_cols) * HD ** (-0.5)
    final_top = jnp.maximum(merged_top, own_score)
    past_scale = jnp.exp(merged_top - final_top)
    own_weight = jnp.exp(own_score - final_top)
    totals = merged_total * past_scale + own_weight
    own_rounded = lax.optimization_barrier(own_weight.astype(jnp.bfloat16)).astype(jnp.float32)
    own_values = jnp.broadcast_to(
        new_value.astype(jnp.float32).reshape(row_count, local_heads, 1, HD),
        (row_count, local_heads, group_size, HD),
    ).reshape(row_count, head_cols * HD)
    weighted = (
        merged_values * jnp.repeat(past_scale, HD, axis=1)
        + jnp.repeat(own_rounded, HD, axis=1) * own_values
    )
    attended = (weighted / jnp.repeat(totals, HD, axis=1)).astype(jnp.bfloat16)
    partial_out = jnp.dot(attended, out_weight, preferred_element_type=jnp.float32)
    head_sum = lax.psum(partial_out.astype(jnp.bfloat16), "tp").astype(jnp.float32)
    mid_cols = (token_rows + head_sum).astype(jnp.bfloat16)
    mid_rows = lax.all_gather(mid_cols, "kv", axis=1, tiled=True)
    mid_wide = mid_rows.astype(jnp.float32)
    normed_mid = (
        mid_wide
        * mlp_gain[None, :]
        * lax.rsqrt(jnp.mean(mid_wide * mid_wide, axis=1, keepdims=True) + epsilon)
    ).astype(jnp.bfloat16)
    hidden = jnp.square(
        jax.nn.relu(jnp.dot(normed_mid, up_weight, preferred_element_type=jnp.float32))
    ).astype(jnp.bfloat16)
    mixer_term = jnp.dot(hidden, down_weight, preferred_element_type=jnp.float32)
    kv_count = lax.axis_size("kv")
    tp_count = lax.axis_size("tp")
    block_cols = mixer_term.shape[1] // (kv_count * tp_count)
    reordered = (
        mixer_term.reshape(row_count, kv_count, tp_count, block_cols)
        .transpose(0, 2, 1, 3)
        .reshape(row_count, kv_count * tp_count * block_cols)
    )
    pair_share = lax.psum_scatter(
        reordered.astype(jnp.bfloat16), "tp", scatter_dimension=1, tiled=True
    ).astype(jnp.float32)
    mixer_share = lax.psum_scatter(pair_share, "kv", scatter_dimension=1, tiled=True)
    out_cols = mixer_share.shape[1]
    start_col = (kv_place * tp_count + tp_place) * out_cols
    mid_share = lax.dynamic_slice_in_dim(mid_wide, start_col, out_cols, 1)
    return (mid_share + mixer_share).astype(jnp.bfloat16)


LANES = 128
SUBLANES = 8
VMEM = pltpu.VMEM
HBM = pltpu.HBM
f32 = jnp.float32
bf16 = jnp.bfloat16
in_vmem = pl.BlockSpec(memory_space=pltpu.VMEM)
in_smem = pl.BlockSpec(memory_space=pltpu.SMEM)
in_hbm = pl.BlockSpec(memory_space=pltpu.HBM)
anywhere = pl.BlockSpec(memory_space=pl.ANY)


HOLD_WORK = 10**10
PROJECT_WORK = 10**8
ATTEND_WORK = 10**10
MERGE_WORK = 10**10
NORM_WORK = 10**8
SPREAD_WORK = 10**8


def call(kernel, outs, in_specs, args, scratch=(), megabytes=8, work=1 << 20, name=None):
    many = isinstance(outs, (list, tuple))
    return pl.pallas_call(
        kernel,
        out_shape=outs,
        in_specs=in_specs,
        out_specs=[in_vmem] * len(outs) if many else in_vmem,
        scratch_shapes=list(scratch),
        compiler_params=pltpu.CompilerParams(vmem_limit_bytes=megabytes * 1024 * 1024),
        cost_estimate=pl.CostEstimate(
            flops=work,
            bytes_accessed=1 << 16,
            transcendentals=0,
        ),
        name=name,
    )(*args)


def pinned(x, space):
    return pltpu.with_memory_space_constraint(x, space)


def round_up(n, m):
    return -(-n // m) * m


def lane_index(rows):
    return lax.broadcasted_iota(jnp.int32, (rows, LANES), 1)


def project_kernel(
    tokens_hbm,
    gain_hbm,
    query_hbm,
    key_hbm,
    value_hbm,
    forget_hbm,
    part_ref,
    tokens,
    gain,
    query,
    key,
    value,
    forget,
    stage,
    sems,
):
    rows, feats = tokens.shape
    chunks = query.shape[0]
    depth = query.shape[1]
    kv_place = lax.axis_index("kv")
    start = pl.multiple_of(kv_place * feats, feats)
    copies = [
        pltpu.make_async_copy(tokens_hbm, tokens, sems.at[0]),
        pltpu.make_async_copy(gain_hbm, gain, sems.at[1]),
        pltpu.make_async_copy(forget_hbm.at[:, pl.ds(start, feats)], forget, sems.at[2]),
        pltpu.make_async_copy(key_hbm, key, sems.at[3]),
        pltpu.make_async_copy(value_hbm, value, sems.at[4]),
    ]
    streams = [
        pltpu.make_async_copy(
            query_hbm.at[pl.ds(i * depth, depth), :], query.at[i], sems.at[5 + i]
        )
        for i in range(chunks)
    ]
    for copy in copies[:2]:
        copy.start()
    for copy in streams:
        copy.start()
    for copy in copies[2:]:
        copy.start()
    for copy in copies[:2]:
        copy.wait()
    token_rows = tokens[...].astype(f32)
    scaled = (token_rows * gain[...]).astype(bf16)
    squares = jnp.sum(token_rows * token_rows, axis=1, keepdims=True)
    total = None
    for i in range(chunks):
        streams[i].wait()
        term = jnp.dot(
            scaled[:, i * depth : (i + 1) * depth], query[i], preferred_element_type=f32
        )
        total = term if total is None else total + term
    for copy in copies[2:]:
        copy.wait()
    key_part = jnp.dot(scaled, key[...], preferred_element_type=f32)
    value_part = jnp.dot(scaled, value[...], preferred_element_type=f32)
    forget_part = lax.dot_general(
        scaled, forget[...], (((1,), (1,)), ((), ())), preferred_element_type=f32
    )
    heads = forget_part.shape[1]
    lane = lane_index(rows)
    extra = jnp.where(lane == heads, squares, 0.0)
    for j in range(heads):
        extra = jnp.where(lane == j, forget_part[:, j : j + 1], extra)
    high = extra.astype(bf16).astype(f32)
    low = extra - high
    extra = high + pltpu.roll(low, LANES // 2, axis=1)
    stage[...] = jnp.zeros(stage.shape, f32)
    tiles = total.shape[1] // LANES
    for c in range(tiles):
        stage[c * rows : (c + 1) * rows, :] = total[:, c * LANES : (c + 1) * LANES]
    for j, block in enumerate((key_part, value_part, extra)):
        stage[(tiles + j) * rows : (tiles + j + 1) * rows, :] = block
    part_ref[...] = stage[...].astype(bf16)


def hold_kernel(count, *refs):
    sources = refs[1 : 1 + count]
    targets = refs[1 + count : 1 + 2 * count]
    sems = refs[1 + 2 * count]
    copies = [
        pltpu.make_async_copy(s, t, sems.at[i])
        for i, (s, t) in enumerate(zip(sources, targets))
    ]
    for copy in copies:
        copy.start()
    for copy in copies:
        copy.wait()


def hold(after, arrays, name):
    outs = [pltpu.VMEM(a.shape, a.dtype) for a in arrays]
    return call(
        functools.partial(hold_kernel, len(arrays)),
        outs,
        [anywhere] + [in_hbm] * len(arrays),
        [after] + [pinned(a, HBM) for a in arrays],
        scratch=[pltpu.SemaphoreType.DMA((len(arrays),))],
        megabytes=1,
        work=HOLD_WORK,
        name=name,
    )


def attend_kernel(
    peers, rows, lengths, offset, keys, values, gates, *refs
):
    parts = refs[:peers]
    sent_ref, stage = refs[peers:]
    positions = keys.shape[1]
    kv_place = lax.axis_index("kv")
    tp_place = lax.axis_index("tp")
    summed = parts[0][...].astype(f32)
    for part in parts[1:]:
        summed = summed + part[...].astype(f32)
    stage[...] = summed
    tiles = HEADS // lax.axis_size("tp") * HD // LANES
    half = tiles // 2
    extra = stage[(tiles + 2) * rows : (tiles + 3) * rows, :]
    extra = extra + pltpu.roll(extra, LANES // 2, axis=1)
    scale = lax.rsqrt(extra[:, KEY_VALUE_HEADS : KEY_VALUE_HEADS + 1] / D + epsilon)
    gate_in = extra * scale
    lane_row = lax.broadcasted_iota(jnp.int32, (tiles, LANES), 1)
    tile_row = lax.broadcasted_iota(jnp.int32, (tiles, LANES), 0)
    low_lane = lane_row < HD
    low_tile = tile_row < half
    mine = low_lane == low_tile
    wide_tile = lax.broadcasted_iota(jnp.int32, (tiles, positions), 0) < half
    place = kv_place * positions + lax.broadcasted_iota(jnp.int32, (2 * tiles, positions), 1)
    owner = kv_place == 0
    stats = jnp.zeros((tiles, LANES), f32)
    for b in range(rows):
        row_scale = scale[b : b + 1, :]
        tile = (stage[pl.ds(b, tiles, stride=rows), :] * row_scale).astype(bf16).astype(f32)
        turned = pltpu.roll(tile, HD, axis=1)
        even = jnp.where(low_tile, tile, turned)
        odd = jnp.where(low_tile, turned, tile)
        even = jnp.where(mine, even, 0.0)
        odd = jnp.where(mine, odd, 0.0)
        query = jnp.concatenate([even, odd], axis=0)
        new_key = (stage[tiles * rows + b : tiles * rows + b + 1, :] * row_scale).astype(bf16)
        new_value = (
            stage[(tiles + 1) * rows + b : (tiles + 1) * rows + b + 1, :] * row_scale
        ).astype(bf16)
        scores = lax.dot_general(
            query.astype(bf16),
            keys[b],
            (((1,), (1,)), ((), ())),
            preferred_element_type=f32,
        ) * HD ** (-0.5)
        both = []
        for g in range(2):
            column = tp_place * 2 + g
            picked = jnp.sum(
                jnp.where(
                    lax.broadcasted_iota(jnp.int32, (1, LANES), 1) == column,
                    gate_in[b : b + 1, :],
                    0.0,
                ),
                axis=1,
                keepdims=True,
            )
            raw = picked + offset[g]
            log_forget = jnp.minimum(raw, 0.0) - jnp.log1p(jnp.exp(-jnp.abs(raw)))
            both.append(gates[b, g : g + 1, :] + log_forget)
        bias = jnp.where(wide_tile, both[0], both[1])
        scores = scores + jnp.concatenate([bias, bias], axis=0)
        live = place < lengths[b]
        scores = jnp.where(live, scores, floor_score)
        own = jnp.sum(query * new_key.astype(f32), axis=1, keepdims=True) * HD ** (-0.5)
        own = jnp.where(owner, own, floor_score)
        top = jnp.maximum(jnp.max(scores, axis=1, keepdims=True), own)
        top_high = top.astype(bf16).astype(f32)
        top_low = (top - top_high).astype(bf16).astype(f32)
        top = top_high + top_low
        weights = jnp.where(live, jnp.exp(scores - top), 0.0)
        own_weight = jnp.where(owner, jnp.exp(own - top), 0.0)
        total = jnp.sum(weights, axis=1, keepdims=True) + own_weight
        total_high = total.astype(bf16).astype(f32)
        total_low = total - total_high
        summed_values = jnp.dot(weights.astype(bf16), values[b], preferred_element_type=f32)
        summed_values = summed_values + own_weight.astype(bf16).astype(f32) * new_value.astype(f32)
        even = summed_values[:tiles]
        odd = summed_values[tiles:]
        placed_even = jnp.where(low_tile, even, pltpu.roll(even, HD, axis=1))
        placed_odd = jnp.where(low_tile, pltpu.roll(odd, HD, axis=1), odd)
        sent_ref[b * tiles : (b + 1) * tiles, :] = jnp.where(
            low_lane, placed_even, placed_odd
        ).astype(bf16)
        for j, column in enumerate((top_high, top_low, total_high, total_low)):
            for parity in range(2):
                stats = jnp.where(
                    lane_row == j * (LANES // 4) + 2 * b + parity,
                    column[parity * tiles : (parity + 1) * tiles],
                    stats,
                )
    sent_ref[rows * tiles :, :] = stats.astype(bf16)


def merge_kernel(peers, rows, *refs):
    parts = refs[:peers]
    attended_ref, stage = refs[peers:]
    tiles = parts[0].shape[0] // (rows + 1)
    quarter = LANES // 4
    tops, totals = [], []
    for part in parts:
        stats = part[rows * tiles :, :].astype(f32)
        tops.append(stats + pltpu.roll(stats, LANES - quarter, axis=1))
        totals.append(
            pltpu.roll(stats, LANES - 2 * quarter, axis=1)
            + pltpu.roll(stats, LANES - 3 * quarter, axis=1)
        )
    top = functools.reduce(jnp.maximum, tops)
    scales = [jnp.exp(t - top) for t in tops]
    total = functools.reduce(jnp.add, [t * s for t, s in zip(totals, scales)])
    shares = [s / total for s in scales]
    low_lane = lane_index(tiles) < HD
    for b in range(rows):
        mixed = None
        for part, share in zip(parts, shares):
            factor = jnp.where(
                low_lane, share[:, 2 * b : 2 * b + 1], share[:, 2 * b + 1 : 2 * b + 2]
            )
            term = part[b * tiles : (b + 1) * tiles, :].astype(f32) * factor
            mixed = term if mixed is None else mixed + term
        stage[b * tiles : (b + 1) * tiles, :] = mixed
    for c in range(tiles):
        attended_ref[:, c * LANES : (c + 1) * LANES] = stage[
            pl.ds(c, rows, stride=tiles), :
        ].astype(bf16)


def norm_kernel(peers, gain, *refs):
    mids = refs[:peers]
    normed_ref, share_ref, ordered = refs[peers:]
    width = mids[0].shape[1]
    cols = share_ref.shape[1]
    kv_place = lax.axis_index("kv")
    tp_place = lax.axis_index("tp")
    wides = [m[...].astype(f32) for m in mids]
    squares = functools.reduce(
        jnp.add, [jnp.sum(w * w, axis=1, keepdims=True) for w in wides]
    )
    scale = lax.rsqrt(squares / D + epsilon)
    for k in range(peers):
        source = kv_place ^ k
        ordered[source] = wides[k] * gain[source] * scale
    for j in range(peers):
        normed_ref[:, j * width : (j + 1) * width] = ordered[j].astype(bf16)
    share_ref[...] = jnp.where(tp_place == 0, wides[0][:, :cols], wides[0][:, cols:])


def spread_kernel(peers, mixed, share, kept_ref, sent_ref, spread):
    blocks, _, cols = spread.shape
    kv_place = lax.axis_index("kv")
    tp_place = lax.axis_index("tp")
    for q in range(blocks):
        spread[q] = mixed[:, q * cols : (q + 1) * cols]
    for k in range(peers):
        target = 2 * (kv_place ^ k)
        own = spread[target + tp_place]
        kept_ref[k] = own + share[...] if k == 0 else own
        sent_ref[k] = spread[target + 1 - tp_place].astype(bf16)


def swap(x, axis, k):
    return lax.ppermute(x, axis, [(i, i ^ k) for i in range(lax.axis_size(axis))])


def shards_direct(
    tokens,
    lengths,
    attn_gain,
    query_weight,
    key_weight,
    value_weight,
    forget_weight,
    forget_offset,
    cache_keys,
    cache_values,
    gate_sum,
    out_weight,
    mlp_gain,
    up_weight,
    down_weight,
):
    rows, feats = tokens.shape
    peers = lax.axis_size("kv")
    others = range(1, peers)
    tiles = query_weight.shape[1] // LANES
    chunks = 4
    depth = feats // chunks
    part_rows = round_up((tiles + 3) * rows, SUBLANES)
    part = call(
        project_kernel,
        jax.ShapeDtypeStruct((part_rows, LANES), bf16),
        [in_hbm] * 6,
        [
            pinned(x, HBM)
            for x in (
                tokens,
                attn_gain.reshape(1, feats),
                query_weight,
                key_weight,
                value_weight,
                forget_weight.T,
            )
        ],
        scratch=[
            pltpu.VMEM((rows, feats), bf16),
            pltpu.VMEM((1, feats), f32),
            pltpu.VMEM((chunks, depth, query_weight.shape[1]), bf16),
            pltpu.VMEM(key_weight.shape, bf16),
            pltpu.VMEM(value_weight.shape, bf16),
            pltpu.VMEM((forget_weight.shape[1], feats), bf16),
            pltpu.VMEM((part_rows, LANES), f32),
            pltpu.SemaphoreType.DMA((5 + chunks,)),
        ],
        megabytes=12,
        work=PROJECT_WORK,
        name="project",
    )
    parts = [part] + [swap(part, "kv", k) for k in others]
    keys_held, values_held, gates_held = hold(
        part, [cache_keys, cache_values, gate_sum], "hold_caches"
    )
    sent = call(
        functools.partial(attend_kernel, peers, rows),
        jax.ShapeDtypeStruct(((rows + 1) * tiles, LANES), bf16),
        [in_smem] * 2 + [in_vmem] * (3 + peers),
        [lengths, forget_offset]
        + [pinned(x, VMEM) for x in (keys_held, values_held, gates_held)]
        + parts,
        scratch=[pltpu.VMEM((part_rows, LANES), f32)],
        megabytes=6,
        work=ATTEND_WORK,
        name="attend",
    )
    sents = [sent] + [swap(sent, "kv", k) for k in others]
    attended = call(
        functools.partial(merge_kernel, peers, rows),
        jax.ShapeDtypeStruct((rows, tiles * LANES), bf16),
        [in_vmem] * peers,
        sents,
        scratch=[pltpu.VMEM((rows * tiles, LANES), f32)],
        megabytes=6,
        work=MERGE_WORK,
        name="merge",
    )
    partial = jnp.dot(attended, out_weight, preferred_element_type=f32).astype(bf16)
    mid = (
        tokens.astype(f32) + partial.astype(f32) + swap(partial, "tp", 1).astype(f32)
    ).astype(bf16)
    mids = [mid] + [swap(mid, "kv", k) for k in others]
    model = down_weight.shape[1]
    blocks = 2 * peers
    cols = model // blocks
    normed, share = call(
        functools.partial(norm_kernel, peers),
        [
            jax.ShapeDtypeStruct((rows, model), bf16),
            jax.ShapeDtypeStruct((rows, cols), f32),
        ],
        [in_vmem] * (1 + peers),
        [mlp_gain.reshape(peers, 1, model // peers)] + mids,
        scratch=[pltpu.VMEM((peers, rows, model // peers), f32)],
        megabytes=4,
        work=NORM_WORK,
        name="norm",
    )
    hidden = jnp.square(
        jax.nn.relu(jnp.dot(normed, up_weight, preferred_element_type=f32))
    ).astype(bf16)
    hidden = lax.optimization_barrier(hidden)
    mixed = jnp.dot(hidden, down_weight, preferred_element_type=f32)
    kept, crossing = call(
        functools.partial(spread_kernel, peers),
        [
            jax.ShapeDtypeStruct((peers, rows, cols), f32),
            jax.ShapeDtypeStruct((peers, rows, cols), bf16),
        ],
        [in_vmem] * 2,
        [mixed, share],
        scratch=[pltpu.VMEM((blocks, rows, cols), f32)],
        megabytes=4,
        work=SPREAD_WORK,
        name="spread",
    )
    paired = kept + swap(crossing, "tp", 1).astype(f32)
    shares = [swap(paired[k].astype(bf16), "kv", k) for k in others]
    result = paired[0]
    for share in shares:
        result = result + share.astype(f32)
    return result.astype(bf16)


def direct_fits(mesh):
    peers = mesh.shape["kv"]
    return mesh.shape["tp"] == 2 and peers in (2, 4) and HD * 2 == LANES


def solution(mesh):
    placed = (
        P("dp", "kv"),
        P("dp"),
        P("kv"),
        P("kv", "tp"),
        P("kv", "tp"),
        P("kv", "tp"),
        P(),
        P("tp"),
        P("dp", "kv", "tp"),
        P("dp", "kv", "tp"),
        P("dp", "tp", "kv"),
        P("tp", "kv"),
        P(),
        P(None, ("kv", "tp")),
        P(("kv", "tp"), None),
    )
    return jax.shard_map(
        shards_direct if direct_fits(mesh) else shards, mesh=mesh, in_specs=placed, out_specs=P("dp", ("kv", "tp")), check_vma=False
    )
```
